32 devices in a mesh: gr: 2 (over x), sp: 8 (over z, y), tp: 2 (over core).
Axes of the slice: x: 2, y: 2, z: 4, core: 2. Of those that a mesh axis runs over, the one named last changes fastest.
Arguments:
- tokens: bfloat16 [8, 2048, 2048], P('gr', 'sp'), parts along dimension 0, may hold values from -6 to 6
- new_rows: bfloat16 [8, 2048], P('gr'), parts along dimension 0, may hold values from -6 to 6
- new_query: bfloat16 [8, 1024], P('gr', 'tp'), parts along dimension 0, may hold values from -6 to 6
- norm_gain: bfloat16 [2048], replicated, may hold values from 0.099609375 to 1.8984375
- key_weight: bfloat16 [2048, 1024], P('sp', 'tp'), may hold values from -0.125 to 0.125
- value_weight: bfloat16 [2048, 2048], P('sp', 'tp'), may hold values from -0.125 to 0.125
- input_weight: bfloat16 [2048, 16], replicated, may hold values from -0.125 to 0.125
- forget_weight: bfloat16 [2048, 16], replicated, may hold values from -0.125 to 0.125
- forget_bias: float32 [16], P('tp'), may hold values from 3 to 12
- gate_offsets: float32 [8, 2048, 2, 16], P('gr', 'sp', None, 'tp'), parts along dimension 0, may hold values from -6 to 250, as said below
Outputs:
- cache_keys: bfloat16 [16, 1024, 1024], P(('gr', 'sp'), None, 'tp'), parts along dimension 0
- cache_values: bfloat16 [16, 1024, 2048], P(('gr', 'sp'), None, 'tp'), parts along dimension 0
- cache_weights: float32 [16, 16, 1024], P(('gr', 'sp'), 'tp'), parts along dimension 0
- first_read: bfloat16 [8, 2048], P('gr', 'tp'), parts along dimension 0
The draws below stay inside these ranges and needn't reach their ends.
There are 2 independent parts, one for each index of `gr`. The reference program is written for one: setup_inputs(seed, part) draws one part's arguments, and reference() takes and returns one part's arrays. A program takes and returns all parts, laid end to end along the dimension named above; an argument that names none is the same for every part. Nothing has to cross between parts.
Inputs may be any that keep to these rules, and one draw needn't show every extreme that they name: `gate_offsets`: entry 1 along the third dimension is never positive.
All inputs are finite; a program needn't handle non-finite values.
Results may differ from the reference program's by a relative error of at most 0.012.
The reference program's roundings to bfloat16 on the way count: a program that leaves them out, or rounds other values in their place, can miss the bound.
Values may be sent and summed in bfloat16 or wider, within the bound.
No kernel may reach another device: no remote copies, remote signals or barrier semaphores. Data moves between devices by JAX's collectives and lax.ppermute only.
A program may use at most 64 MiB of HBM per device.

```python
import math
import jax
import jax.numpy as jnp
from jax import lax

D = 2048
HEADS = 16
DK = 64
DV = 128
SEQS = 4
CONTEXT_SPAN = 2048
PIECES = 2
SUB = 128
N_SP = 8


def draw_forget_bias(key, part):
    pick_key, slow_key, fast_key = jax.random.split(key, 3)
    fast_share = 0.5
    is_fast = jax.random.uniform(pick_key, (HEADS,), jnp.float32) < fast_share
    slow_bias = math.log(3.3 * CONTEXT_SPAN) + jax.random.uniform(slow_key, (HEADS,), jnp.float32, -0.3, 0.3)
    fast_bias = math.log(60.0) + jax.random.uniform(fast_key, (HEADS,), jnp.float32, -0.5, 0.5)
    return jnp.where(is_fast, fast_bias, slow_bias).astype(jnp.float32)


def draw_gate_offsets(key, part):
    incomplete_key_vectors = jax.random.split(key, 4)
    tensor_dimension_count = (SEQS, CONTEXT_SPAN, HEADS)
    block_rate = jnp.exp(jax.random.uniform(incomplete_key_vectors[0], (SEQS, CONTEXT_SPAN // 32, HEADS), jnp.float32, math.log(0.25), 0.0))
    entire_throughput = jnp.repeat(block_rate, 32, axis=1)
    transfer_aligned = jax.random.uniform(incomplete_key_vectors[1], tensor_dimension_count, jnp.float32) < 2.0 / CONTEXT_SPAN
    transfer_span = jnp.log(jax.random.uniform(incomplete_key_vectors[2], tensor_dimension_count, jnp.float32, 0.5, 0.8))
    forgetting_shift = -entire_throughput / CONTEXT_SPAN + jnp.where(transfer_aligned, transfer_span, 0.0)
    input_shift = jnp.clip(jax.random.normal(incomplete_key_vectors[3], tensor_dimension_count, jnp.float32), -6.0, 6.0)
    return jnp.stack([input_shift, forgetting_shift], axis=2).astype(jnp.float32)


def shard_levels(key, extent, cuts, low, high):
    def one(dim, shards_of):
        steps = jax.random.uniform(jax.random.fold_in(jax.random.fold_in(key, 6), dim), (shards_of,), jnp.float32, low / len(cuts), high / len(cuts))
        return jnp.repeat(jnp.exp(steps), extent[dim] // shards_of).reshape((-1,) + (1,) * (len(extent) - dim - 1))

    level = one(*cuts[0])
    for cut in cuts[1:]:
        level = level * one(*cut)
    return level


def noise(rng, extent, spread, bound, cuts=(), dtype=jnp.bfloat16):
    factor_of = shard_levels(rng, extent, cuts, -0.22, 0.18) if cuts else 1.0
    result = jax.random.normal(rng, extent, jnp.float32) * spread * factor_of
    return jnp.minimum(jnp.maximum(result, -bound), bound).astype(dtype)


def setup_inputs(seed: int = 0, part: int = 0) -> dict:
    seeds = jax.random.split(jax.random.key(seed), 11)
    part_keys = jax.random.split(jax.random.fold_in(seeds[10], part), 11)
    tokens = noise(part_keys[0], (SEQS, CONTEXT_SPAN, D), 1.0, 6.0, ((1, 8),))
    new_rows = noise(part_keys[1], (SEQS, D), 1.0, 6.0)
    new_query = noise(part_keys[2], (SEQS, HEADS * DK), 1.0, 6.0, ((1, 2),))
    norm_gain = jnp.clip(1.0 + 0.18 * jax.random.normal(seeds[3], (D,), jnp.float32), 0.099609375, 1.8984375).astype(jnp.bfloat16)
    key_weight = noise(seeds[4], (D, HEADS * DK), D ** -0.5, 0.125, ((0, 8), (1, 2)))
    value_weight = noise(seeds[5], (D, HEADS * DV), D ** -0.5, 0.125, ((0, 8), (1, 2)))
    input_weight = noise(seeds[6], (D, HEADS), D ** -0.5, 0.125)
    forget_weight = noise(seeds[7], (D, HEADS), D ** -0.5, 0.125)
    forget_bias = draw_forget_bias(jax.random.fold_in(seeds[10], 71), part)
    gate_offsets = draw_gate_offsets(jax.random.fold_in(jax.random.fold_in(seeds[10], part), 71), part)
    return {"tokens": tokens, "new_rows": new_rows, "new_query": new_query, "norm_gain": norm_gain, "key_weight": key_weight, "value_weight": value_weight, "input_weight": input_weight, "forget_weight": forget_weight, "forget_bias": forget_bias, "gate_offsets": gate_offsets}


EPSILON = 1e-06

def normed_rows(source, norm_gain):
    widened = source.astype(jnp.float32)
    inverse_rms = lax.rsqrt(lax.optimization_barrier(jnp.mean(widened * widened, axis=-1, keepdims=True)) + EPSILON)
    return (widened * inverse_rms * norm_gain.astype(jnp.float32)).astype(jnp.bfloat16)

def suffix_sums(log_forget):
    flipped = jnp.cumsum(jnp.flip(log_forget, 1), axis=1)
    return jnp.flip(flipped, 1) - log_forget

def cache_order(rows):
    width = rows.shape[-1]
    split = rows.reshape(SEQS, N_SP, PIECES, SUB, width)
    return jnp.transpose(split, (0, 2, 1, 3, 4)).reshape(SEQS * PIECES, N_SP * SUB, width)

def reference(tokens, new_rows, new_query, norm_gain, key_weight, value_weight, input_weight, forget_weight, forget_bias, gate_offsets):
    seq_count = tokens.shape[0]
    flat_rows = normed_rows(tokens, norm_gain).reshape(seq_count * CONTEXT_SPAN, D)
    key_rows = (jnp.dot(flat_rows, key_weight, preferred_element_type=jnp.float32) * DK ** (-0.5)).astype(jnp.bfloat16)
    value_rows = jnp.dot(flat_rows, value_weight, preferred_element_type=jnp.float32).astype(jnp.bfloat16)
    input_gate = jnp.dot(flat_rows, input_weight, preferred_element_type=jnp.float32).reshape(seq_count, CONTEXT_SPAN, HEADS) + gate_offsets[:, :, 0, :]
    forget_pre = jnp.dot(flat_rows, forget_weight, preferred_element_type=jnp.float32).reshape(seq_count, CONTEXT_SPAN, HEADS)
    log_forget = jax.nn.log_sigmoid(forget_pre + forget_bias) + gate_offsets[:, :, 1, :]
    log_weight = input_gate + suffix_sums(log_forget)
    peak_log = lax.optimization_barrier(jnp.max(log_weight, axis=1))
    query_heads = new_query.reshape(seq_count, HEADS, DK).astype(jnp.float32)
    key_heads = key_rows.reshape(seq_count, CONTEXT_SPAN, HEADS, DK).astype(jnp.float32)
    value_heads = value_rows.reshape(seq_count, CONTEXT_SPAN, HEADS, DV).astype(jnp.float32)
    scores = jnp.einsum('nhd,nshd->nsh', query_heads, key_heads)
    weighted_terms = jnp.exp(log_weight - peak_log[:, None, :]) * scores
    rounded = lax.optimization_barrier(weighted_terms.astype(jnp.bfloat16)).astype(jnp.float32)
    numerator = jnp.einsum('nsh,nshd->nhd', rounded, value_heads)
    denominator = lax.optimization_barrier(jnp.sum(weighted_terms, axis=1))
    fresh_rows = normed_rows(new_rows, norm_gain)
    key_new = (jnp.dot(fresh_rows, key_weight, preferred_element_type=jnp.float32) * DK ** (-0.5)).astype(jnp.bfloat16)
    value_new = jnp.dot(fresh_rows, value_weight, preferred_element_type=jnp.float32).astype(jnp.bfloat16)
    gate_new = jnp.dot(fresh_rows, input_weight, preferred_element_type=jnp.float32)
    peak_new = jnp.maximum(peak_log, gate_new)
    old_part = jnp.exp(peak_log - peak_new)
    own_score = jnp.einsum('nhd,nhd->nh', query_heads, key_new.reshape(seq_count, HEADS, DK).astype(jnp.float32))
    new_part = jnp.exp(gate_new - peak_new) * own_score
    total_value = old_part[..., None] * numerator + new_part[..., None] * value_new.reshape(seq_count, HEADS, DV).astype(jnp.float32)
    total_weight = old_part * denominator + new_part
    read_out = total_value / jnp.maximum(jnp.abs(total_weight), 1.0)[..., None]
    return (cache_order(key_rows.reshape(seq_count, CONTEXT_SPAN, HEADS * DK)), cache_order(value_rows.reshape(seq_count, CONTEXT_SPAN, HEADS * DV)), jnp.transpose(cache_order(log_weight), (0, 2, 1)), read_out.reshape(seq_count, HEADS * DV).astype(jnp.bfloat16))
```

```python
import functools

import jax
import jax.numpy as jnp
from jax import lax
from jax.experimental import pallas as pl
from jax.experimental.pallas import tpu as pltpu
from jax.sharding import PartitionSpec as P

EPSILON = 1e-06


def normed_rows(source, norm_gain):
    widened = source.astype(jnp.float32)
    inverse_rms = lax.rsqrt(jnp.mean(widened * widened, axis=-1, keepdims=True) + EPSILON)
    return (widened * inverse_rms * norm_gain.astype(jnp.float32)).astype(jnp.bfloat16)


def pick(parts, index):
    out = parts[0]
    for k in range(1, len(parts)):
        out = jnp.where(index == k, parts[k], out)
    return out


def ring(x, axis, size, shift):
    return lax.ppermute(x, axis, [(i, (i + shift) % size) for i in range(size)])


def project_kernel(
    first, key_cols, scale, heads, value_size,
    place, x, w, query, logs, peak, *rest,
):
    if first:
        fresh, keys, values, part, new = rest
    else:
        _, _, before, keys, values, part = rest
    rows = x.shape[0]
    sums = jnp.dot(x[...], w[...], preferred_element_type=jnp.float32)
    k = (sums[:, :key_cols] * scale).astype(jnp.bfloat16)
    v = sums[:, key_cols:].astype(jnp.bfloat16)
    keys[...] = k
    values[...] = v
    scores = lax.dot_general(
        query[...], k, (((1,), (1,)), ((), ())), preferred_element_type=jnp.float32
    )
    terms = jnp.exp(logs[...] - peak[...]) * scores
    top = jnp.dot(terms.astype(jnp.bfloat16), v, preferred_element_type=jnp.float32)
    below = jnp.sum(terms, axis=1, keepdims=True)
    for h in range(heads):
        num = top[h : h + 1, h * value_size : (h + 1) * value_size]
        den = jnp.broadcast_to(below[h : h + 1], (1, value_size))
        if first:
            part[h : h + 1] = num
            part[heads + h : heads + h + 1] = den
        else:
            part[h : h + 1] = before[h : h + 1] + num
            part[heads + h : heads + h + 1] = before[heads + h : heads + h + 1] + den
    if first:
        new[...] = jnp.dot(fresh[...], w[...], preferred_element_type=jnp.float32)


def project(place, x, w, query, logs, peak, extra, total, key_cols, heads, scale):
    first = len(extra) == 1
    rows = x.shape[0]
    value_cols = w.shape[1] - key_cols
    value_size = value_cols // heads
    whole = pl.BlockSpec(memory_space=pltpu.VMEM)
    in_specs = [
        whole,
        whole,
        whole,
        pl.BlockSpec((heads, rows), lambda i, at: (0, at[0])),
        whole,
    ]
    out_shape = [
        jax.ShapeDtypeStruct((total, key_cols), jnp.bfloat16),
        jax.ShapeDtypeStruct((total, value_cols), jnp.bfloat16),
        jax.ShapeDtypeStruct((2 * heads, value_size), jnp.float32),
    ]
    out_specs = [
        pl.BlockSpec((rows, key_cols), lambda i, at: (at[0], 0)),
        pl.BlockSpec((rows, value_cols), lambda i, at: (at[0], 0)),
        whole,
    ]
    aliases = {}
    if first:
        in_specs += [whole]
        out_shape += [jax.ShapeDtypeStruct((extra[0].shape[0], w.shape[1]), jnp.float32)]
        out_specs += [whole]
    else:
        in_specs += [pl.BlockSpec(memory_space=pl.ANY), pl.BlockSpec(memory_space=pl.ANY), whole]
        aliases = {6: 0, 7: 1}
    return pl.pallas_call(
        functools.partial(project_kernel, first, key_cols, scale, heads, value_size),
        out_shape=out_shape,
        grid_spec=pltpu.PrefetchScalarGridSpec(
            num_scalar_prefetch=1, grid=(1,), in_specs=in_specs, out_specs=out_specs
        ),
        input_output_aliases=aliases,
        compiler_params=pltpu.CompilerParams(dimension_semantics=("arbitrary",)),
    )(place, x, w, query, logs, peak, *extra)


def per_device(
    tokens,
    new_rows,
    new_query,
    norm_gain,
    key_weight,
    value_weight,
    input_weight,
    forget_weight,
    forget_bias,
    gate_offsets,
):
    seqs, positions, width = tokens.shape
    heads = forget_bias.shape[0]
    key_cols, value_cols = key_weight.shape[1], value_weight.shape[1]
    key_size, value_size = key_cols // heads, value_cols // heads
    groups, group_size, cores = (lax.axis_size(a) for a in ("gr", "sp", "tp"))
    pieces = group_size // seqs
    sub = positions // pieces
    g, s, t = (lax.axis_index(a) for a in ("gr", "sp", "tp"))
    n, p = s // pieces, s % pieces

    def along(x, shift):
        return lax.ppermute(
            x, "sp",
            [(i, (i // pieces + shift) % seqs * pieces + i % pieces) for i in range(group_size)],
        )

    def across(x, shift):
        return lax.ppermute(
            x, "sp",
            [(i, i // pieces * pieces + (i % pieces + shift) % pieces) for i in range(group_size)],
        )

    depth = key_weight.shape[0]
    share = depth // groups
    own = jnp.concatenate([key_weight, value_weight], axis=1)
    held = {(0, 0): lax.dynamic_slice_in_dim(own, g * share, share, 0)}
    held[1, 0] = along(held[0, 0], 1)
    if seqs > 2:
        held[seqs - 1, 0] = along(held[0, 0], -1)
    for k in range(2, seqs - 1):
        held[k, 0] = along(held[k - 1, 0], 1)
    order = [0, 1, seqs - 1] + list(range(2, seqs - 1))
    for k in order:
        for q in range(1, pieces):
            held[k, q] = across(held[k, q - 1], 1)
    weight = jnp.zeros((width, key_cols + value_cols), jnp.bfloat16)
    for k in order:
        for q in range(pieces):
            base = ((n - k) % seqs * pieces + (p - q) % pieces) * depth
            if (k, q) == (0, 0):
                weight = lax.dynamic_update_slice_in_dim(weight, own, base, 0)
                continue
            part = held[k, q]
            for c in range(groups):
                if c:
                    part = ring(part, "gr", groups, 1)
                weight = lax.dynamic_update_slice_in_dim(
                    weight, part, base + (g - c) % groups * share, 0
                )

    normed = normed_rows(tokens, norm_gain)
    mine = lax.dynamic_slice_in_dim(
        normed.reshape(seqs, pieces, cores, sub // cores, width), t, 1, 2
    )[:, :, 0]
    gathered = [lax.dynamic_index_in_dim(mine, p, 1, keepdims=False)]
    for q in range(1, pieces):
        gathered.append(
            across(lax.dynamic_index_in_dim(mine, (p + q) % pieces, 1, keepdims=False), q)
        )
    bundle = jnp.stack([pick(gathered, (p - q) % pieces) for q in range(pieces)], axis=1)

    rows = normed.reshape(seqs * positions, width)
    fresh_all = normed_rows(new_rows, norm_gain)
    start = t * heads
    gate_weight = jnp.concatenate(
        [
            lax.dynamic_slice_in_dim(input_weight, start, heads, 1),
            lax.dynamic_slice_in_dim(forget_weight, start, heads, 1),
        ],
        axis=1,
    )
    sums = lax.dot_general(
        gate_weight, rows, (((0,), (1,)), ((), ())), preferred_element_type=jnp.float32
    ).reshape(2, heads, seqs, positions)
    offsets = jnp.transpose(gate_offsets, (2, 3, 0, 1))
    input_gate = sums[0] + offsets[0]
    log_forget = jax.nn.log_sigmoid(sums[1] + forget_bias[:, None, None]) + offsets[1]
    later = jnp.flip(jnp.cumsum(jnp.flip(log_forget, 2), axis=2), 2) - log_forget
    local = input_gate + later
    stats = jnp.stack([jnp.sum(log_forget, axis=2), jnp.max(local, axis=2)])
    lines = -(-stats.size // sub)
    line = jnp.pad(stats.reshape(-1), (0, lines * sub - stats.size)).reshape(1, lines, sub)
    send = jnp.concatenate(
        [
            jnp.transpose(local.reshape(heads, seqs * pieces, sub), (1, 0, 2)),
            jnp.broadcast_to(line, (group_size, lines, sub)),
        ],
        axis=1,
    )
    got = lax.all_to_all(send, "sp", split_axis=0, concat_axis=0, tiled=True)
    all_stats = got[:, heads:].reshape(group_size, -1)[:, : stats.size]
    all_stats = all_stats.reshape((group_size,) + stats.shape)
    tails = [jnp.zeros_like(stats[0])]
    for j in range(group_size - 1, 0, -1):
        tails.append(tails[-1] + all_stats[j, 0])
    tails = jnp.stack(tails[::-1])
    tops = jnp.max(tails + all_stats[:, 1], axis=0)
    tail = lax.dynamic_index_in_dim(tails, n, 2, keepdims=False)
    peak = lax.dynamic_index_in_dim(tops, n, 1, keepdims=True)
    logs = jnp.transpose(got[:, :heads] + tail[:, :, None], (1, 0, 2)).reshape(heads, -1)

    fresh = lax.dynamic_slice_in_dim(fresh_all, n, 1, 0)
    query = lax.dynamic_slice_in_dim(new_query, n, 1, 0)
    head_of = lax.broadcasted_iota(jnp.int32, (heads, key_cols), 1) // key_size
    lead = lax.broadcasted_iota(jnp.int32, (heads, key_cols), 0)
    spread = jnp.where(head_of == lead, query, jnp.zeros_like(query))
    fresh_block = jnp.broadcast_to(fresh, (16, width))

    total = group_size * sub
    keys = values = part = new = None
    for k in order:
        block = lax.dynamic_index_in_dim(bundle, (n + k) % seqs, 0, keepdims=False)
        if k:
            block = along(block, k if 2 * k <= seqs else k - seqs)
        shares = [block]
        for c in range(1, cores):
            shares.append(ring(block, "tp", cores, c))
        block = jnp.stack([pick(shares, (t - c) % cores) for c in range(cores)], axis=1)
        block = block.reshape(pieces * sub, width)
        place = ((n - k) % seqs).astype(jnp.int32).reshape(1)
        extra = (fresh_block,) if keys is None else (keys, values, part)
        made = project(
            place, block, weight, spread, logs, peak, extra, total, key_cols, heads,
            key_size ** (-0.5),
        )
        if keys is None:
            keys, values, part, new = made
        else:
            keys, values, part = made

    summed = part
    for q in range(1, pieces):
        summed = summed + across(part, q)
    numerator, denominator = summed[:heads], summed[heads:, :1]
    new = new[:1]
    key_new = (new[:, :key_cols] * key_size ** (-0.5)).astype(jnp.bfloat16)
    value_new = new[:, key_cols:].astype(jnp.bfloat16).astype(jnp.float32)
    gate_new = jnp.dot(fresh, gate_weight[:, :heads], preferred_element_type=jnp.float32)
    gate_new = gate_new.reshape(heads, 1)
    peak_new = jnp.maximum(peak, gate_new)
    old_part = jnp.exp(peak - peak_new)
    own_score = jnp.sum(
        spread.astype(jnp.float32) * key_new.astype(jnp.float32), axis=1, keepdims=True
    )
    new_part = jnp.exp(gate_new - peak_new) * own_score
    above = old_part * numerator + new_part * value_new.reshape(heads, value_size)
    below = old_part * denominator + new_part
    read = (above / jnp.maximum(jnp.abs(below), 1.0)).astype(jnp.bfloat16)
    reads = [read] + [along(read, k) for k in range(1, seqs)]
    out = jnp.stack([pick(reads, (n - k) % seqs) for k in range(seqs)])
    return (
        keys[None],
        values[None],
        logs[None],
        out.reshape(seqs, heads * value_size),
    )


def solution(mesh):
    return jax.shard_map(
        per_device,
        mesh=mesh,
        in_specs=(
            P("gr", "sp", None),
            P("gr", None),
            P("gr", "tp"),
            P(),
            P("sp", "tp"),
            P("sp", "tp"),
            P(),
            P(),
            P("tp"),
            P("gr", "sp", None, "tp"),
        ),
        out_specs=(
            P(("gr", "sp"), None, "tp"),
            P(("gr", "sp"), None, "tp"),
            P(("gr", "sp"), "tp", None),
            P("gr", "tp"),
        ),
        check_vma=False,
    )
```
